32 devices in a mesh: ep: 16 (over z, x, core), tp: 2 (over y).
Axes of the slice: x: 2, y: 2, z: 4, core: 2. Of those that a mesh axis runs over, the one named last changes fastest.
Arguments:
- tokens: bfloat16 [2048, 2048], P('ep'), may hold values from -6 to 6
- routes: int32 [2048, 2], P('ep'), may hold values from 0 to 3, all different within a row; in each aligned block of 128 rows (0 to 127, 128 to 255, ...) at most 80 rows name the same one
- router_weight: bfloat16 [2048, 4], replicated, may hold values from -0.125 to 0.125
- gate_proj: bfloat16 [16, 2048, 1024], P('ep', None, 'tp'), may hold values from -0.125 to 0.125
- up_proj: bfloat16 [16, 2048, 1024], P('ep', None, 'tp'), may hold values from -0.125 to 0.125
- down_proj: bfloat16 [16, 1024, 2048], P('ep', 'tp'), may hold values from -0.09375 to 0.09375
- cotangent: bfloat16 [2048, 2048], P('ep'), may hold values from -1.5 to 1.5
Outputs:
- token_grad: bfloat16 [2048, 2048], P('ep', 'tp')
- gate_grad: float32 [2048, 2], P('ep')
- router_grad: float32 [2048, 4], P('ep')
- gate_proj_grad: float32 [16, 2048, 1024], P('ep', None, 'tp')
- up_proj_grad: float32 [16, 2048, 1024], P('ep', None, 'tp')
- down_proj_grad: float32 [16, 1024, 2048], P('ep', 'tp')
The draws below stay inside these ranges and needn't reach their ends.
Inputs may be any that keep to these rules, and one draw needn't show every extreme that they name: `routes`: each row names 2 different experts. Among the rows of one index of ep no expert is named more than 80 times, a bound that some block reaches.
All inputs are finite; a program needn't handle non-finite values.
Results may differ from the reference program's by a relative error of at most 0.0085.
Values may be sent and summed in bfloat16 or wider, within the bound.
A program may use at most 128 MiB of HBM per device.

```python
import math
import jax
import jax.numpy as jnp
import numpy as np
from jax import lax

D = 2048
FF = 4096
MEMBERS = 4
TOP = 2
TOK_DEV = 128
BLOCK_FF = 1024
EXPERTS = 4
CAP = 80
TOKENS = 2048
N_EP = 16


def levels(stream_key, shape, shards, smallest, top_value):
    factor_of = 1.0
    for axis_at, blocks in shards:
        steps = jax.random.uniform(jax.random.fold_in(jax.random.fold_in(stream_key, 6), axis_at), (blocks,), jnp.float32, smallest / len(shards), top_value / len(shards))
        factor_of = factor_of * jnp.repeat(jnp.exp(steps), shape[axis_at] // blocks).reshape((-1,) + (1,) * (len(shape) - 1 - axis_at))
    return factor_of


def routed_block(stream_key, own, number, rows, count, top, most, lean):
    order = jax.random.permutation(stream_key, count)
    packed, common = shares(count, rows * top, most, lean, True), shares(count, rows * top, most, lean, False)
    places = jnp.arange(count)

    def named(sizes, rotation):
        used = int((sizes > 0).sum())
        fixed = max(1, used // 4)
        moved = fixed + (places - fixed + rotation * (used - fixed)) % max(1, count - fixed)
        return jnp.zeros((count,), jnp.int32).at[order[jnp.where(places < fixed, places, moved)]].set(jnp.asarray(sizes, jnp.int32))

    sizes = jnp.where(number % 4 == 0, named(packed, number // 4), named(common, number - number // 4 - 1))
    mixed = jax.random.permutation(jax.random.fold_in(own, 3), count)
    donor, taker = mixed[0:count // 2 * 2:2], mixed[1:count // 2 * 2:2]
    slack = jnp.minimum(sizes[donor] - 1, most - sizes[taker]) // 2
    slack = jnp.where((donor == order[0]) | (taker == order[0]) | (sizes[taker] == 0), 0, jnp.maximum(slack, 0))
    moved = jax.random.randint(jax.random.fold_in(own, 4), (count // 2,), 0, 1 << 20) % (slack + 1)
    sizes = sizes.at[donor].add(-moved).at[taker].add(moved)
    items = jnp.searchsorted(jnp.cumsum(sizes), jnp.arange(rows * top), side="right").astype(jnp.int32)
    table = items.reshape(top, rows).T
    table = table[jax.random.permutation(jax.random.fold_in(own, 1), rows)]
    rotation = jax.random.randint(jax.random.fold_in(own, 2), (rows, 1), 0, top)
    return jnp.take_along_axis(table, (jnp.arange(top)[None, :] + rotation) % top, axis=1)


def shares(number_of, total, limit, slope, full):
    loads = [(1 << 20) // math.isqrt(rank ** slope) + 1 for rank in range(1, number_of + 1)]
    largest = limit if full else min(limit, max(-(-total // number_of), total * loads[0] // sum(loads)))
    least = 1 if total - largest >= number_of - 1 else 0
    holding, surplus = [largest] + [least] * (number_of - 1), total - largest - least * (number_of - 1)
    while surplus > 0:
        free = [i for i in range(1, number_of) if holding[i] < largest] or [i for i in range(1, number_of) if holding[i] < limit]
        pool, budget = sum([loads[i] for i in free]), surplus
        for i in free:
            addition = min(limit - holding[i], max(1, budget * loads[i] // pool), surplus)
            holding[i] = holding[i] + addition
            surplus = surplus - addition
    return np.array(holding)


def scatter_about(stream_key, shape, width, limit, pieces=(), held_as=jnp.bfloat16):
    result = width * jax.random.normal(stream_key, shape, jnp.float32)
    if pieces:
        result = result * levels(stream_key, shape, pieces, -0.22, 0.18)
    return jnp.clip(result, -limit, limit).astype(held_as)


def setup_inputs(seed: int = 0) -> dict:
    key_list = jax.random.split(jax.random.key(seed), 8)
    tokens = scatter_about(key_list[0], (TOKENS, D), 1.0, 6.0, ((0, 16),))
    routes_keys = jax.random.split(jax.random.fold_in(key_list[1], 1), TOKENS // TOK_DEV)
    routes_turns = jax.random.permutation(jax.random.fold_in(key_list[1], 3), TOKENS // TOK_DEV)
    routes = jax.vmap(lambda own, number: routed_block(jax.random.fold_in(key_list[1], 2), own, number, TOK_DEV, EXPERTS, TOP, CAP, 2))(routes_keys, routes_turns).reshape((TOKENS, TOP))
    router_weight = scatter_about(key_list[2], (D, EXPERTS), D ** -0.5, 0.125)
    gate_proj = scatter_about(key_list[3], (EXPERTS * MEMBERS, D, BLOCK_FF), D ** -0.5, 0.125, ((0, 16), (2, 2)))
    up_proj = scatter_about(key_list[4], (EXPERTS * MEMBERS, D, BLOCK_FF), D ** -0.5, 0.125, ((0, 16), (2, 2)))
    down_proj = scatter_about(key_list[5], (EXPERTS * MEMBERS, BLOCK_FF, D), FF ** -0.5, 0.09375, ((0, 16), (1, 2)))
    cotangent = scatter_about(key_list[6], (TOKENS, D), 0.25, 1.5, ((0, 16),))
    return dict(tokens=tokens, routes=routes, router_weight=router_weight, gate_proj=gate_proj, up_proj=up_proj, down_proj=down_proj, cotangent=cotangent)


def expert_backward(tok_rows, cot_rows, gate_rows, w_gate, w_up, w_down):
    gpre = jnp.dot(tok_rows, w_gate, preferred_element_type=jnp.float32)
    upre = jnp.dot(tok_rows, w_up, preferred_element_type=jnp.float32)
    sig = jax.nn.sigmoid(gpre)
    silu_val = gpre * sig
    hidden = (silu_val * upre).astype(jnp.bfloat16)
    qvals = lax.dot_general(cot_rows, w_down, (((1,), (1,)), ((), ())), preferred_element_type=jnp.float32)
    gate_part = jnp.sum(hidden.astype(jnp.float32) * qvals, axis=1)
    weight = gate_rows[:, None]
    dhid = weight * qvals
    d_gate = (dhid * upre * sig * (1.0 + gpre * (1.0 - sig))).astype(jnp.bfloat16)
    d_up = (dhid * silu_val).astype(jnp.bfloat16)
    scaled = (weight * hidden.astype(jnp.float32)).astype(jnp.bfloat16)
    grad_down = lax.dot_general(scaled, cot_rows, (((0,), (0,)), ((), ())), preferred_element_type=jnp.float32)
    grad_gate = lax.dot_general(tok_rows, d_gate, (((0,), (0,)), ((), ())), preferred_element_type=jnp.float32)
    grad_up = lax.dot_general(tok_rows, d_up, (((0,), (0,)), ((), ())), preferred_element_type=jnp.float32)
    row_grad = lax.dot_general(d_gate, w_gate, (((1,), (1,)), ((), ())), preferred_element_type=jnp.float32)
    row_grad = row_grad + lax.dot_general(d_up, w_up, (((1,), (1,)), ((), ())), preferred_element_type=jnp.float32)
    return grad_gate, grad_up, grad_down, row_grad, gate_part


def reference(tokens, routes, router_weight, gate_proj, up_proj, down_proj, cotangent):
    ntok = tokens.shape[0]
    experts = router_weight.shape[1]
    slots = N_EP * CAP
    logits = jnp.dot(tokens, router_weight, preferred_element_type=jnp.float32)
    onehot = (routes[:, :, None] == jnp.arange(experts, dtype=jnp.int32)[None, None, :]).astype(jnp.float32)
    chosen = jnp.sum(onehot * logits[:, None, :], axis=2)
    first = jax.nn.sigmoid(chosen[:, 0] - chosen[:, 1])
    gates = jnp.stack([first, 1.0 - first], axis=1)
    used = lax.optimization_barrier(gates.astype(jnp.bfloat16)).astype(jnp.float32)
    flat = onehot.reshape(N_EP, TOK_DEV * TOP, experts)
    rank = jnp.cumsum(flat, axis=1) - flat
    rank_sel = jnp.sum(flat * rank, axis=2).reshape(ntok, TOP).astype(jnp.int32)
    source = (jnp.arange(ntok, dtype=jnp.int32) // TOK_DEV)[:, None]
    target = routes * slots + source * CAP + rank_sel
    token_ids = jnp.broadcast_to(jnp.arange(ntok, dtype=jnp.int32)[:, None], (ntok, TOP))
    slot_token = jnp.full((experts * slots,), ntok, jnp.int32).at[target.reshape(-1)].set(token_ids.reshape(-1))
    slot_gate = jnp.zeros((experts * slots,), jnp.float32).at[target.reshape(-1)].set(used.reshape(-1))
    slot_token = slot_token.reshape(experts, slots)
    slot_gate = slot_gate.reshape(experts, slots)
    zero_row = jnp.zeros((1, D), jnp.bfloat16)
    pad_tok = jnp.concatenate([tokens, zero_row], axis=0)
    pad_cot = jnp.concatenate([cotangent, zero_row], axis=0)
    full_gate = gate_proj.reshape(experts, MEMBERS, D, BLOCK_FF).transpose(0, 2, 1, 3).reshape(experts, D, FF)
    full_up = up_proj.reshape(experts, MEMBERS, D, BLOCK_FF).transpose(0, 2, 1, 3).reshape(experts, D, FF)
    full_down = down_proj.reshape(experts, FF, D)

    def one_expert(items):
        ids, gate_rows, w_gate, w_up, w_down = items
        return expert_backward(pad_tok[ids], pad_cot[ids], gate_rows, w_gate, w_up, w_down)

    grad_gate, grad_up, grad_down, row_grads, gate_parts = lax.map(
        one_expert, (slot_token, slot_gate, full_gate, full_up, full_down))
    route_sum = jax.ops.segment_sum(row_grads.reshape(-1, D), slot_token.reshape(-1), num_segments=ntok + 1)[:ntok]
    gate_grad = gate_parts.reshape(-1)[target]
    delta = first * (1.0 - first) * (gate_grad[:, 0] - gate_grad[:, 1])
    dlogits = delta[:, None] * (onehot[:, 0] - onehot[:, 1])
    router_part = jnp.dot(dlogits, router_weight.astype(jnp.float32).T, precision=lax.Precision.HIGHEST)
    token_grad = (route_sum + router_part).astype(jnp.bfloat16)
    router_grad = jnp.dot(tokens.astype(jnp.float32).T, dlogits, precision=lax.Precision.HIGHEST)
    gate_proj_grad = grad_gate.reshape(experts, D, MEMBERS, BLOCK_FF).transpose(0, 2, 1, 3).reshape(experts * MEMBERS, D, BLOCK_FF)
    up_proj_grad = grad_up.reshape(experts, D, MEMBERS, BLOCK_FF).transpose(0, 2, 1, 3).reshape(experts * MEMBERS, D, BLOCK_FF)
    down_proj_grad = grad_down.reshape(experts * MEMBERS, BLOCK_FF, D)
    return token_grad, gate_grad, router_grad, gate_proj_grad, up_proj_grad, down_proj_grad
```

```python
import functools

import jax
import jax.numpy as jnp
from jax import lax
from jax.experimental import pallas as pl
from jax.experimental.pallas import tpu as pltpu
from jax.sharding import Mesh, PartitionSpec as P

MEMBERS = 4
TOP = 2
LANES = 128
F32 = jnp.float32
BF16 = jnp.bfloat16
NT = (((1,), (1,)), ((), ()))


def rows_kernel(share, x_ref, wg_ref, wu_ref, wd_ref, dg_ref, du_ref, sc_ref, back_ref):
    n_tp = x_ref.shape[1]
    experts = lax.axis_size("e")
    e_idx = lax.axis_index("e")

    def contract(base, w_ref, dims):
        total = None
        for t in range(n_tp):
            part = x_ref[0, t, :, base : base + share]
            if dims is None:
                term = jnp.dot(part, w_ref[0, t * share : (t + 1) * share, :], preferred_element_type=F32)
            else:
                term = lax.dot_general(
                    part, w_ref[0, :, t * share : (t + 1) * share], dims, preferred_element_type=F32
                )
            total = term if total is None else total + term
        return total

    gpre = contract(0, wg_ref, None)
    upre = contract(0, wu_ref, None)
    qvals = contract(share, wd_ref, NT)
    extra = x_ref[0, 0, :, 2 * share :].astype(F32)
    lane = lax.broadcasted_iota(jnp.int32, extra.shape, 1)
    weight = jnp.sum(jnp.where(lane == experts + e_idx, extra, 0.0), axis=1, keepdims=True)
    sig = jax.nn.sigmoid(gpre)
    silu_val = gpre * sig
    hidden = (silu_val * upre).astype(BF16).astype(F32)
    gate_part = jnp.sum(hidden * qvals, axis=1, keepdims=True)
    dhid = weight * qvals
    d_gate = (dhid * upre * sig * (1.0 + gpre * (1.0 - sig))).astype(BF16)
    d_up = (dhid * silu_val).astype(BF16)
    dg_ref[0] = d_gate
    du_ref[0] = d_up
    sc_ref[0] = (weight * hidden).astype(BF16)
    gate_lanes = jnp.where(lane == e_idx, gate_part, 0.0).astype(BF16)
    for t in range(n_tp):
        cols = slice(t * share, (t + 1) * share)
        grad = lax.dot_general(d_gate, wg_ref[0, cols, :], NT, preferred_element_type=F32)
        grad = grad + lax.dot_general(d_up, wu_ref[0, cols, :], NT, preferred_element_type=F32)
        back_ref[0, t, :, :share] = grad.astype(BF16)
        back_ref[0, t, :, share:] = gate_lanes


def grads_kernel(x_ref, c_ref, dg_ref, du_ref, sc_ref, gg_ref, gu_ref, gd_ref, sct):
    @pl.when(pl.program_id(0) == 0)
    def _():
        sct[...] = sc_ref[...].T

    tile = x_ref.shape[-1]
    rows = dg_ref.shape[0]
    xt = x_ref[:, 0].reshape(rows, tile).T
    gg_ref[0] = jnp.dot(xt, dg_ref[...], preferred_element_type=F32)
    gu_ref[0] = jnp.dot(xt, du_ref[...], preferred_element_type=F32)
    gd_ref[0] = jnp.dot(sct[...], c_ref[:, 0].reshape(rows, tile), preferred_element_type=F32)


def shards(tokens, routes, router_weight, gate_proj, up_proj, down_proj, cotangent):
    ntok, width = tokens.shape
    experts = router_weight.shape[1]
    n_m, n_tp = lax.axis_size("m"), lax.axis_size("tp")
    share = width // n_tp
    capacity = min(ntok, 5 * TOP * ntok // (4 * experts))
    tp_index = lax.axis_index("tp")
    e_index = lax.axis_index("e")
    ff = gate_proj.shape[2]

    logits = jnp.dot(tokens, router_weight, preferred_element_type=F32)
    onehot = (routes[:, :, None] == jnp.arange(experts, dtype=jnp.int32)[None, None, :]).astype(F32)
    chosen = jnp.sum(onehot * logits[:, None, :], axis=2)
    first = jax.nn.sigmoid(chosen[:, 0] - chosen[:, 1])
    gates = jnp.stack([first, 1.0 - first], axis=1)
    used = gates.astype(BF16)
    named = jnp.sum(onehot, axis=1)
    below = (jnp.arange(ntok)[:, None] > jnp.arange(ntok)[None, :]).astype(BF16)
    rank = jnp.dot(below, named.astype(BF16), preferred_element_type=F32)
    slot_cols = jnp.where(named > 0, rank, 255.0).astype(BF16)
    gate_cols = jnp.sum(onehot * used.astype(F32)[:, :, None], axis=1).astype(BF16)
    extras = jnp.concatenate(
        [slot_cols, gate_cols, jnp.zeros((ntok, LANES - 2 * experts), BF16)], axis=1
    )
    send = jnp.concatenate(
        [
            lax.dynamic_slice_in_dim(tokens, tp_index * share, share, 1),
            lax.dynamic_slice_in_dim(cotangent, tp_index * share, share, 1),
            extras,
        ],
        axis=1,
    )
    near = lax.all_gather(send, "e", axis=0, tiled=False)
    lanes = jnp.arange(LANES)[None, None, :]
    slot = jnp.sum(jnp.where(lanes == e_index, near[:, :, 2 * share :].astype(F32), 0.0), axis=2)
    place = (
        jnp.arange(capacity, dtype=jnp.int32)[None, :, None] == slot.astype(jnp.int32)[:, None, :]
    ).astype(BF16)
    rows = jnp.einsum("ect,etw->ecw", place, near, preferred_element_type=F32).astype(BF16)
    held = experts * capacity
    wide = 2 * share + LANES
    full = lax.all_gather(rows.reshape(held, wide), ("m", "tp"), axis=0, tiled=False)
    full = full.reshape(n_m, n_tp, held, wide)

    back_wide = share + LANES
    hid_spec = pl.BlockSpec((1, held, ff), lambda i: (i, 0, 0))
    hid_shape = jax.ShapeDtypeStruct((n_m, held, ff), BF16)
    flops = 2 * n_m * held * width * ff
    d_gate, d_up, scaled, back = pl.pallas_call(
        functools.partial(rows_kernel, share),
        grid=(n_m,),
        in_specs=[
            pl.BlockSpec((1, n_tp, held, wide), lambda i: (i, 0, 0, 0)),
            pl.BlockSpec((1, width, ff), lambda i: (0, 0, 0)),
            pl.BlockSpec((1, width, ff), lambda i: (0, 0, 0)),
            pl.BlockSpec((1, ff, width), lambda i: (0, 0, 0)),
        ],
        out_specs=[
            hid_spec,
            hid_spec,
            hid_spec,
            pl.BlockSpec((1, n_tp, held, back_wide), lambda i: (i, 0, 0, 0)),
        ],
        out_shape=[
            hid_shape,
            hid_shape,
            hid_shape,
            jax.ShapeDtypeStruct((n_m, n_tp, held, back_wide), BF16),
        ],
        cost_estimate=pl.CostEstimate(flops=5 * flops, bytes_accessed=30 << 20, transcendentals=0),
        name="rows",
    )(full, gate_proj, up_proj, down_proj)

    mine = lax.psum_scatter(
        back.reshape(n_m * n_tp, held, back_wide), ("m", "tp"), scatter_dimension=0, tiled=False
    )

    tile = 256
    per = share // tile
    total = n_m * held
    whole = lambda i: (0, 0)
    grad_gate, grad_up, grad_down = pl.pallas_call(
        grads_kernel,
        grid=(width // tile,),
        in_specs=[
            pl.BlockSpec((n_m, 1, held, tile), lambda i: (0, i // per, 0, i % per)),
            pl.BlockSpec((n_m, 1, held, tile), lambda i: (0, i // per, 0, per + i % per)),
            pl.BlockSpec((total, ff), whole),
            pl.BlockSpec((total, ff), whole),
            pl.BlockSpec((total, ff), whole),
        ],
        out_specs=[
            pl.BlockSpec((1, tile, ff), lambda i: (0, i, 0)),
            pl.BlockSpec((1, tile, ff), lambda i: (0, i, 0)),
            pl.BlockSpec((1, ff, tile), lambda i: (0, 0, i)),
        ],
        out_shape=[
            jax.ShapeDtypeStruct(gate_proj.shape, F32),
            jax.ShapeDtypeStruct(up_proj.shape, F32),
            jax.ShapeDtypeStruct(down_proj.shape, F32),
        ],
        scratch_shapes=[pltpu.VMEM((ff, total), BF16)],
        cost_estimate=pl.CostEstimate(flops=3 * flops, bytes_accessed=30 << 20, transcendentals=0),
        name="grads",
    )(full, full, d_gate.reshape(total, ff), d_up.reshape(total, ff), scaled.reshape(total, ff))

    dense = jnp.einsum(
        "ect,ecw->etw",
        place,
        mine.reshape(experts, capacity, back_wide),
        preferred_element_type=F32,
    ).astype(BF16)
    home = lax.psum_scatter(dense, "e", scatter_dimension=0, tiled=False).astype(F32)
    route_sum = home[:, :share]
    gate_grad = jnp.sum(onehot * home[:, None, share : share + experts], axis=2)
    delta = first * (1.0 - first) * (gate_grad[:, 0] - gate_grad[:, 1])
    dlogits = delta[:, None] * (onehot[:, 0] - onehot[:, 1])
    router_rows = lax.dynamic_slice_in_dim(router_weight, tp_index * share, share, 0).astype(F32)
    router_part = lax.dot_general(dlogits, router_rows, NT, precision=lax.Precision.HIGHEST)
    token_grad = (route_sum + router_part).astype(BF16)
    n_ep = lax.axis_size("e") * n_m
    terms = lax.dot_general(
        dlogits, tokens.astype(F32), (((0,), (0,)), ((), ())), precision=lax.Precision.HIGHEST
    )
    terms = terms.reshape(experts, n_ep, width // n_ep).transpose(1, 0, 2)
    terms = lax.all_to_all(terms, ("e", "m"), split_axis=0, concat_axis=0, tiled=True)
    router_grad = jnp.sum(terms, axis=0).T
    return (token_grad, gate_grad, router_grad, grad_gate, grad_up, grad_down)


def solution(mesh):
    devices = mesh.devices
    grid = Mesh(
        devices.reshape(devices.shape[0] // MEMBERS, MEMBERS, devices.shape[1]), ("e", "m", "tp")
    )
    ep = ("e", "m")
    return jax.shard_map(
        shards,
        mesh=grid,
        in_specs=(
            P(ep, None),
            P(ep, None),
            P(),
            P(ep, None, "tp"),
            P(ep, None, "tp"),
            P(ep, "tp", None),
            P(ep, None),
        ),
        out_specs=(
            P(ep, "tp"),
            P(ep, None),
            P(ep, None),
            P(ep, None, "tp"),
            P(ep, None, "tp"),
            P(ep, "tp", None),
        ),
        check_vma=False,
    )
```

```python
import functools

import jax
import jax.numpy as jnp
from jax import lax
from jax.experimental import pallas as pl
from jax.experimental.pallas import tpu as pltpu
from jax.sharding import Mesh, PartitionSpec as P

MEMBERS = 4
TOP = 2
LANES = 128
F32 = jnp.float32
BF16 = jnp.bfloat16
MESH = pl.DeviceIdType.MESH
NT = (((1,), (1,)), ((), ()))


def rows_kernel(
    share, send_ref, wg_hbm, wu_hbm, wd_hbm, x_hbm, dg_ref, du_ref, sc_ref, back_ref,
    full, wg_ref, wu_ref, wd_ref, out_sem, send_sem, recv_sem, load_sem,
):
    experts, n_m, n_tp, capacity, _ = full.shape
    e, m, t = lax.axis_index("e"), lax.axis_index("m"), lax.axis_index("tp")
    x_peer = lax.rem(m + 2, 4)
    core_peer = m + 1 - 2 * lax.rem(m, 2)
    held = n_m * capacity
    first_cols, last_cols = pl.ds(0, share), pl.ds(share, share + LANES)

    def ahead(j):
        return lax.rem(t + j, n_tp)

    def behind(j):
        return lax.rem(t + n_tp - j, n_tp)

    barrier = pltpu.get_barrier_semaphore()
    peers = [(lax.rem(e + k, experts), m, t) for k in range(1, experts)]
    peers += [(e, x_peer, t), (e, core_peer, t)] + [(e, m, ahead(j)) for j in range(1, n_tp)]
    for peer in peers:
        pl.semaphore_signal(barrier, inc=1, device_id=peer, device_id_type=MESH)
    loads = [
        pltpu.make_async_copy(src, dst, load_sem.at[n])
        for n, (src, dst) in enumerate(
            [(send_ref.at[e], full.at[0, m, t]), (wg_hbm, wg_ref), (wu_hbm, wu_ref), (wd_hbm, wd_ref)]
        )
    ]
    for load in loads:
        load.start()
    pl.semaphore_wait(barrier, len(peers))

    def remote(src, dst, kind, k, device):
        return pltpu.make_async_remote_copy(
            src_ref=src,
            dst_ref=dst,
            send_sem=send_sem.at[kind, k],
            recv_sem=recv_sem.at[kind, k],
            device_id=device,
            device_id_type=MESH,
        )

    def piece(k, src_m, src_t, cols=None):
        ref = full.at[k, src_m, src_t]
        return ref if cols is None else ref.at[:, cols]

    X, CORE_OWN, CORE_X = 0, 1, 2
    def y_kind(j): return 3 + (j - 1)
    def a_kind(j): return 3 + (n_tp - 1) + (j - 1)
    def b_kind(j): return 3 + 2 * (n_tp - 1) + (j - 1)
    def core_y(j): return 3 + 3 * (n_tp - 1) + (j - 1)
    def core_a(j): return 3 + 4 * (n_tp - 1) + (j - 1)
    def core_b(j): return 3 + 5 * (n_tp - 1) + (j - 1)
    Z = 3 + 6 * (n_tp - 1)

    def pass_on(ref, kind, k, device):
        remote(ref, ref, kind, k, device).start()

    def landed(ref, kind, k):
        remote(ref, ref, kind, k, (e, core_peer, t)).wait_recv()

    def sent(ref, kind, k):
        remote(ref, ref, kind, k, (e, core_peer, t)).wait_send()

    for k in range(1, experts):
        there = lax.rem(e + k, experts)
        remote(send_ref.at[there], full.at[k, m, t], Z, k, (there, m, t)).start()
    loads[0].wait()

    x_to, core_to = (e, x_peer, t), (e, core_peer, t)

    def own(k):
        mine = piece(k, m, t)
        @pl.when(k > 0)
        def _():
            landed(mine, Z, k)
        pass_on(mine, X, k, x_to)
        for j in range(1, n_tp):
            pass_on(mine, y_kind(j), k, (e, m, ahead(j)))
        pass_on(mine, CORE_OWN, k, core_to)

    def neighbours(k):
        across = piece(k, x_peer, t)
        landed(across, X, k)
        for j in range(1, n_tp):
            pass_on(piece(k, x_peer, t, last_cols), b_kind(j), k, (e, m, ahead(j)))
        pass_on(across, CORE_X, k, core_to)
        for j in range(1, n_tp):
            beside = piece(k, m, behind(j))
            landed(beside, y_kind(j), k)
            pass_on(piece(k, m, behind(j), first_cols), a_kind(j), k, x_to)
            pass_on(beside, core_y(j), k, core_to)

    def corners(k):
        for j in range(1, n_tp):
            for cols, kind, core in ((first_cols, a_kind, core_a), (last_cols, b_kind, core_b)):
                ref = piece(k, x_peer, behind(j), cols)
                landed(ref, kind(j), k)
                pass_on(ref, core(j), k, core_to)

    other_x = lax.rem(core_peer + 2, 4)

    def partner(k):
        landed(piece(k, core_peer, t), CORE_OWN, k)
        landed(piece(k, other_x, t), CORE_X, k)
        for j in range(1, n_tp):
            landed(piece(k, core_peer, behind(j)), core_y(j), k)
            landed(piece(k, other_x, behind(j), first_cols), core_a(j), k)
            landed(piece(k, other_x, behind(j), last_cols), core_b(j), k)
        pltpu.make_async_copy(full.at[k], x_hbm.at[k], out_sem.at[k]).start()

    def compute(k):
        def part(tp_at, base, size):
            return full[k, :, tp_at, :, base : base + size].reshape(held, size)

        def contract(base, w_ref, nt):
            total = None
            for tp_at in range(n_tp):
                cols = slice(tp_at * share, (tp_at + 1) * share)
                rows = part(tp_at, base, share)
                if nt:
                    term = lax.dot_general(rows, w_ref[0, :, cols], NT, preferred_element_type=F32)
                else:
                    term = jnp.dot(rows, w_ref[0, cols, :], preferred_element_type=F32)
                total = term if total is None else total + term
            return total

        gpre = contract(0, wg_ref, False)
        upre = contract(0, wu_ref, False)
        qvals = contract(share, wd_ref, True)
        extra = part(0, 2 * share, LANES).astype(F32)
        lane = lax.broadcasted_iota(jnp.int32, extra.shape, 1)
        weight = jnp.sum(jnp.where(lane == e, extra, 0.0), axis=1, keepdims=True)
        sig = jax.nn.sigmoid(gpre)
        silu_val = gpre * sig
        hidden = (silu_val * upre).astype(BF16).astype(F32)
        gate_part = jnp.sum(hidden * qvals, axis=1, keepdims=True)
        dhid = weight * qvals
        d_gate = (dhid * upre * sig * (1.0 + gpre * (1.0 - sig))).astype(BF16)
        d_up = (dhid * silu_val).astype(BF16)
        dg_ref[k] = d_gate
        du_ref[k] = d_up
        sc_ref[k] = (weight * hidden).astype(BF16)
        gate_lanes = jnp.where(lane == 0, gate_part, 0.0).astype(BF16)
        source = lax.rem(e + experts - k, experts)
        for tp_at in range(n_tp):
            cols = slice(tp_at * share, (tp_at + 1) * share)
            grad = lax.dot_general(d_gate, wg_ref[0, cols, :], NT, preferred_element_type=F32)
            grad = grad + lax.dot_general(d_up, wu_ref[0, cols, :], NT, preferred_element_type=F32)
            back_ref[:, tp_at, source, :, :share] = grad.astype(BF16).reshape(n_m, capacity, share)
            back_ref[:, tp_at, source, :, share:] = gate_lanes.reshape(n_m, capacity, LANES)

    def step(i, carry):
        pl.when(i < experts)(lambda: own(i))
        pl.when((i >= 1) & (i < experts + 1))(lambda: neighbours(i - 1))
        pl.when((i >= 2) & (i < experts + 2))(lambda: corners(i - 2))

        @pl.when(i == 3)
        def _():
            for load in loads[1:]:
                load.wait()

        @pl.when(i >= 3)
        def _():
            partner(i - 3)
            compute(i - 3)

        return carry

    lax.fori_loop(0, experts + 3, step, 0)

    def finish(k, carry):
        mine = piece(k, m, t)
        @pl.when(k > 0)
        def _():
            sent(mine, Z, k)
        sent(mine, X, k)
        sent(mine, CORE_OWN, k)
        sent(piece(k, x_peer, t), CORE_X, k)
        for j in range(1, n_tp):
            sent(mine, y_kind(j), k)
            sent(piece(k, x_peer, t, last_cols), b_kind(j), k)
            sent(piece(k, m, behind(j), first_cols), a_kind(j), k)
            sent(piece(k, m, behind(j)), core_y(j), k)
            sent(piece(k, x_peer, behind(j), first_cols), core_a(j), k)
            sent(piece(k, x_peer, behind(j), last_cols), core_b(j), k)
        pltpu.make_async_copy(full.at[k], x_hbm.at[k], out_sem.at[k]).wait()
        return carry

    lax.fori_loop(0, experts, finish, 0)


def grads_kernel(x_ref, c_ref, dg_ref, du_ref, sc_ref, gg_ref, gu_ref, gd_ref, sct):
    @pl.when(pl.program_id(0) == 0)
    def _():
        sct[...] = sc_ref[...].T

    tile = x_ref.shape[-1]
    rows = dg_ref.shape[0]
    xt = x_ref[:, :, 0].reshape(rows, tile).T
    gg_ref[0] = jnp.dot(xt, dg_ref[...], preferred_element_type=F32)
    gu_ref[0] = jnp.dot(xt, du_ref[...], preferred_element_type=F32)
    gd_ref[0] = jnp.dot(sct[...], c_ref[:, :, 0].reshape(rows, tile), preferred_element_type=F32)


def shards(tokens, routes, router_weight, gate_proj, up_proj, down_proj, cotangent):
    ntok, width = tokens.shape
    experts = router_weight.shape[1]
    n_m, n_tp = lax.axis_size("m"), lax.axis_size("tp")
    share = width // n_tp
    capacity = min(ntok, 5 * TOP * ntok // (4 * experts))
    capacity = -(-capacity // 16) * 16
    tp_index = lax.axis_index("tp")
    ff = gate_proj.shape[2]

    logits = jnp.dot(tokens, router_weight, preferred_element_type=F32)
    onehot = (routes[:, :, None] == jnp.arange(experts, dtype=jnp.int32)[None, None, :]).astype(F32)
    chosen = jnp.sum(onehot * logits[:, None, :], axis=2)
    first = jax.nn.sigmoid(chosen[:, 0] - chosen[:, 1])
    gates = jnp.stack([first, 1.0 - first], axis=1)
    used = gates.astype(BF16)
    named = jnp.sum(onehot, axis=1)
    below = (jnp.arange(ntok)[:, None] > jnp.arange(ntok)[None, :]).astype(BF16)
    rank = jnp.dot(below, named.astype(BF16), preferred_element_type=F32)
    slot = jnp.where(named > 0, rank, -1.0).astype(jnp.int32)
    place = (
        jnp.arange(capacity, dtype=jnp.int32)[None, :, None] == slot.T[:, None, :]
    ).astype(BF16)
    gate_cols = jnp.sum(onehot * used.astype(F32)[:, :, None], axis=1).astype(BF16)
    payload = jnp.concatenate(
        [
            lax.dynamic_slice_in_dim(tokens, tp_index * share, share, 1),
            lax.dynamic_slice_in_dim(cotangent, tp_index * share, share, 1),
            gate_cols,
            jnp.zeros((ntok, LANES - experts), BF16),
        ],
        axis=1,
    )
    rows = jnp.dot(
        place.reshape(experts * capacity, ntok), payload, preferred_element_type=F32
    ).astype(BF16)
    wide = 2 * share + LANES
    rows = rows.reshape(experts, capacity, wide)

    held = n_m * capacity
    back_wide = share + LANES
    hid_shape = jax.ShapeDtypeStruct((experts, held, ff), BF16)
    flops = 2 * experts * held * width * ff
    kinds = 4 + 6 * (n_tp - 1)
    vmem = pl.BlockSpec(memory_space=pltpu.VMEM)
    anywhere = pl.BlockSpec(memory_space=pl.ANY)
    full_shape = (experts, n_m, n_tp, capacity, wide)
    full, d_gate, d_up, scaled, back = pl.pallas_call(
        functools.partial(rows_kernel, share),
        in_specs=[vmem, anywhere, anywhere, anywhere],
        out_specs=[anywhere, vmem, vmem, vmem, vmem],
        out_shape=[
            jax.ShapeDtypeStruct(full_shape, BF16),
            hid_shape,
            hid_shape,
            hid_shape,
            jax.ShapeDtypeStruct((n_m, n_tp, experts, capacity, back_wide), BF16),
        ],
        scratch_shapes=[
            pltpu.VMEM(full_shape, BF16),
            pltpu.VMEM(gate_proj.shape, BF16),
            pltpu.VMEM(up_proj.shape, BF16),
            pltpu.VMEM(down_proj.shape, BF16),
            pltpu.SemaphoreType.DMA((experts,)),
            pltpu.SemaphoreType.DMA((kinds, experts)),
            pltpu.SemaphoreType.DMA((kinds, experts)),
            pltpu.SemaphoreType.DMA((4,)),
        ],
        compiler_params=pltpu.CompilerParams(
            collective_id=0, has_side_effects=True, vmem_limit_bytes=60 << 20
        ),
        cost_estimate=pl.CostEstimate(flops=5 * flops, bytes_accessed=30 << 20, transcendentals=0),
        name="rows",
    )(rows, gate_proj, up_proj, down_proj)

    mine = lax.psum_scatter(
        back.reshape(n_m * n_tp, experts * capacity, back_wide),
        ("m", "tp"),
        scatter_dimension=0,
        tiled=False,
    )

    tile = 256
    per = share // tile
    total = experts * held
    whole = lambda i: (0, 0)
    grad_gate, grad_up, grad_down = pl.pallas_call(
        grads_kernel,
        grid=(width // tile,),
        in_specs=[
            pl.BlockSpec((experts, n_m, 1, capacity, tile), lambda i: (0, 0, i // per, 0, i % per)),
            pl.BlockSpec((experts, n_m, 1, capacity, tile), lambda i: (0, 0, i // per, 0, per + i % per)),
            pl.BlockSpec((total, ff), whole),
            pl.BlockSpec((total, ff), whole),
            pl.BlockSpec((total, ff), whole),
        ],
        out_specs=[
            pl.BlockSpec((1, tile, ff), lambda i: (0, i, 0)),
            pl.BlockSpec((1, tile, ff), lambda i: (0, i, 0)),
            pl.BlockSpec((1, ff, tile), lambda i: (0, 0, i)),
        ],
        out_shape=[
            jax.ShapeDtypeStruct(gate_proj.shape, F32),
            jax.ShapeDtypeStruct(up_proj.shape, F32),
            jax.ShapeDtypeStruct(down_proj.shape, F32),
        ],
        scratch_shapes=[pltpu.VMEM((ff, total), BF16)],
        cost_estimate=pl.CostEstimate(flops=3 * flops, bytes_accessed=30 << 20, transcendentals=0),
        name="grads",
    )(full, full, d_gate.reshape(total, ff), d_up.reshape(total, ff), scaled.reshape(total, ff))

    home = lax.all_to_all(
        mine.reshape(experts, capacity, back_wide), "e", split_axis=0, concat_axis=0, tiled=True
    )
    route_sum = lax.dot_general(
        place.reshape(experts * capacity, ntok),
        home[:, :, :share].reshape(experts * capacity, share),
        (((0,), (0,)), ((), ())),
        preferred_element_type=F32,
    )
    gate_at = jnp.einsum(
        "ect,ecl->etl", place, home[:, :, share:], preferred_element_type=F32
    )[:, :, 0]
    gate_grad = jnp.sum(onehot * gate_at.T[:, None, :], axis=2)
    delta = first * (1.0 - first) * (gate_grad[:, 0] - gate_grad[:, 1])
    dlogits = delta[:, None] * (onehot[:, 0] - onehot[:, 1])
    router_rows = lax.dynamic_slice_in_dim(router_weight, tp_index * share, share, 0).astype(F32)
    router_part = lax.dot_general(dlogits, router_rows, NT, precision=lax.Precision.HIGHEST)
    token_grad = (route_sum + router_part).astype(BF16)
    n_ep = lax.axis_size("e") * n_m
    terms = lax.dot_general(
        dlogits, tokens.astype(F32), (((0,), (0,)), ((), ())), precision=lax.Precision.HIGHEST
    )
    terms = terms.reshape(experts, n_ep, width // n_ep).transpose(1, 0, 2)
    terms = lax.all_to_all(terms, ("e", "m"), split_axis=0, concat_axis=0, tiled=True)
    router_grad = jnp.sum(terms, axis=0).T
    return (token_grad, gate_grad, router_grad, grad_gate, grad_up, grad_down)


def solution(mesh):
    devices = mesh.devices
    grid = Mesh(
        devices.reshape(devices.shape[0] // MEMBERS, MEMBERS, devices.shape[1]), ("e", "m", "tp")
    )
    ep = ("e", "m")
    return jax.shard_map(
        shards,
        mesh=grid,
        in_specs=(
            P(ep, None),
            P(ep, None),
            P(),
            P(ep, None, "tp"),
            P(ep, None, "tp"),
            P(ep, "tp", None),
            P(ep, None),
        ),
        out_specs=(
            P(ep, "tp"),
            P(ep, None),
            P(ep, None),
            P(ep, None, "tp"),
            P(ep, None, "tp"),
            P(ep, "tp", None),
        ),
        check_vma=False,
    )
```
